256 devices in a mesh: sp: 32 (over z, y), fs: 4 (over x), tp: 2 (over core).
Axes of the slice: x: 4, y: 4, z: 8, core: 2. Of those that a mesh axis runs over, the one named last changes fastest.
Arguments:
- tokens: bfloat16 [4, 8192, 2048], P('fs', 'sp', 'tp'), may hold values from -6 to 6
- norm_gain: float32 [2048], replicated, may hold values from 0.1 to 1.9
- memory_query: bfloat16 [2048, 1024], P('fs', 'tp'), may hold values from -0.125 to 0.125
- memory_key: bfloat16 [2048, 1024], P('fs', 'tp'), may hold values from -0.125 to 0.125
- memory_value: bfloat16 [2048, 1024], P('fs', 'tp'), may hold values from -0.125 to 0.125
- memory_outgate: bfloat16 [2048, 1024], P('fs', 'tp'), may hold values from -0.125 to 0.125
- memory_ingate: bfloat16 [2048, 4], P(None, 'tp'), may hold values from -0.125 to 0.125
- memory_forget: bfloat16 [2048, 4], P(None, 'tp'), may hold values from -0.125 to 0.125
- forget_bias: float32 [4], P('tp'), may hold values from 3 to 13
- forget_shift: float32 [4, 8192, 4], P('fs', 'sp', 'tp'), may hold values from -1.6 to 0
- stick_query: bfloat16 [2048, 512], P(None, 'tp'), may hold values from -0.125 to 0.125
- stick_key: bfloat16 [2048, 512], P(None, 'tp'), may hold values from -0.125 to 0.125
- stick_value: bfloat16 [2048, 512], P(None, 'tp'), may hold values from -0.125 to 0.125
- stick_bias: float32 [4], P('tp'), may hold values from -11 to -2
- memory_gain: float32 [1024], P('tp'), may hold values from 0.1 to 1.9
- stick_gain: float32 [512], P('tp'), may hold values from 0.1 to 1.9
- out_memory: bfloat16 [1024, 2048], P('tp'), may hold values from -0.15625 to 0.15625
- out_stick: bfloat16 [512, 2048], P('tp'), may hold values from -0.15625 to 0.15625
Outputs:
- mixed: bfloat16 [4, 8192, 2048], P('fs', ('sp', 'tp'))
The draws below stay inside these ranges and needn't reach their ends.
All inputs are finite; a program needn't handle non-finite values.
Results may differ from the reference program's by a relative error of at most 0.015.
Values may be sent and summed in bfloat16 or wider, within the bound.
No kernel may reach another device: no remote copies, remote signals or barrier semaphores. Data moves between devices by JAX's collectives and lax.ppermute only.
A program may use at most 128 MiB of HBM per device.

```python
import jax
import jax.numpy as jnp
from jax import lax

D = 2048
HM = 4
DM = 256
HS = 4
DS = 128
TOK_DEV = 256
BLOCK = 128
SEQ = 8192
SEQS = 4
N_SP = 32


def draw_forget_bias(key, part):
    keys = jax.random.split(jax.random.fold_in(key, 11), 3)
    order = jax.random.permutation(keys[0], HM)
    fast_value = jax.random.uniform(keys[1], (HM,), jnp.float32, 3.0, 4.5)
    slow_value = jnp.log(jnp.float32(SEQ)) + jax.random.uniform(keys[2], (HM,), jnp.float32, 1.0, 2.0)
    return jnp.where(order < HM // 2, slow_value, fast_value)


def draw_forget_shift(key, part):
    keys = jax.random.split(jax.random.fold_in(key, 23), 3)
    spans = SEQ // TOK_DEV
    rate = jax.random.uniform(keys[0], (SEQS, spans, 1, HM), jnp.float32, 0.1, 1.0)
    constant_baseline = -jnp.broadcast_to(rate, (SEQS, spans, TOK_DEV, HM)).reshape(SEQS, SEQ, HM) / jnp.float32(SEQ)
    spots = jax.random.randint(keys[1], (SEQS, 3), 0, SEQ)
    layer_total = jnp.log(jax.random.uniform(keys[2], (SEQS, 3, HM), jnp.float32, 0.6, 0.8))
    pairing_tally = (jnp.arange(SEQ)[None, None, :] == spots[:, :, None]).astype(jnp.float32)
    segment_bundles = jnp.einsum('fwz,fwx->fzx', pairing_tally, layer_total)
    return constant_baseline + segment_bundles


def draw_stick_bias(key, part):
    keys = jax.random.split(jax.random.fold_in(key, 37), 3)
    order = jax.random.permutation(keys[0], HS)
    far_value = -jnp.log(jnp.float32(SEQ)) + jax.random.uniform(keys[1], (HS,), jnp.float32, -0.5, 0.5)
    near_value = jax.random.uniform(keys[2], (HS,), jnp.float32, -4.0, -2.0)
    return jnp.where(order < HS // 2, far_value, near_value)


def shard_levels(rng, dims, cuts, smallest, high):
    def one(axis_at, parts):
        draws = jax.random.uniform(jax.random.fold_in(jax.random.fold_in(rng, 6), axis_at), (parts,), jnp.float32, smallest / len(cuts), high / len(cuts))
        return jnp.repeat(jnp.exp(draws), dims[axis_at] // parts).reshape((-1,) + (1,) * (len(dims) - axis_at - 1))

    factor_of = one(*cuts[0])
    for cut in cuts[1:]:
        factor_of = factor_of * one(*cut)
    return factor_of


def centred(own_key, extent, scale, bound, pieces=(), kind=jnp.bfloat16):
    level = shard_levels(own_key, extent, pieces, -0.22, 0.18) if pieces else 1.0
    result = jax.random.normal(own_key, extent, jnp.float32) * scale * level
    return jnp.minimum(jnp.maximum(result, -bound), bound).astype(kind)


def setup_inputs(seed: int = 0) -> dict:
    key_list = jax.random.split(jax.random.key(seed), 19)
    return {
        "tokens": centred(key_list[0], (SEQS, SEQ, D), 1.0, 6.0, ((0, 4), (1, 32), (2, 2))),
        "norm_gain": jnp.clip(1.0 + 0.18 * jax.random.normal(key_list[1], (D,), jnp.float32), 0.1, 1.9),
        "memory_query": centred(key_list[2], (D, HM * DM), D ** -0.5, 0.125, ((0, 4), (1, 2))),
        "memory_key": centred(key_list[3], (D, HM * DM), D ** -0.5, 0.125, ((0, 4), (1, 2))),
        "memory_value": centred(key_list[4], (D, HM * DM), D ** -0.5, 0.125, ((0, 4), (1, 2))),
        "memory_outgate": centred(key_list[5], (D, HM * DM), D ** -0.5, 0.125, ((0, 4), (1, 2))),
        "memory_ingate": centred(key_list[6], (D, HM), D ** -0.5, 0.125, ((1, 2),)),
        "memory_forget": centred(key_list[7], (D, HM), D ** -0.5, 0.125, ((1, 2),)),
        "forget_bias": draw_forget_bias(jax.random.fold_in(key_list[18], 71), 0),
        "forget_shift": draw_forget_shift(jax.random.fold_in(key_list[18], 71), 0),
        "stick_query": centred(key_list[10], (D, HS * DS), D ** -0.5, 0.125, ((1, 2),)),
        "stick_key": centred(key_list[11], (D, HS * DS), D ** -0.5, 0.125, ((1, 2),)),
        "stick_value": centred(key_list[12], (D, HS * DS), D ** -0.5, 0.125, ((1, 2),)),
        "stick_bias": draw_stick_bias(jax.random.fold_in(key_list[18], 71), 0),
        "memory_gain": jnp.clip(1.0 + 0.18 * jax.random.normal(key_list[14], (HM * DM,), jnp.float32), 0.1, 1.9),
        "stick_gain": jnp.clip(1.0 + 0.18 * jax.random.normal(key_list[15], (HS * DS,), jnp.float32), 0.1, 1.9),
        "out_memory": centred(key_list[16], (HM * DM, D), (HM * DM + HS * DS) ** -0.5, 0.15625, ((0, 2),)),
        "out_stick": centred(key_list[17], (HS * DS, D), (HM * DM + HS * DS) ** -0.5, 0.15625, ((0, 2),)),
    }


epsilon = 1e-06
floor_neg = -1e+30
peak_value = lax.Precision.HIGHEST

def rounded(values):
    return lax.optimization_barrier(values.astype(jnp.bfloat16)).astype(jnp.float32)

def per_head_norm(values, gain):
    scale = lax.rsqrt(lax.optimization_barrier(jnp.mean(values * values, axis=-1, keepdims=True)) + epsilon)
    return values * scale * gain

def memory_block(state_carry, inputs):
    state_matrix, state_max = state_carry
    queries, key_rows, value_rows, log_forget, in_gate = inputs
    length = queries.shape[0]
    causal = jnp.tril(jnp.ones((length, length), dtype=bool))
    cumulative = jnp.cumsum(log_forget, axis=0)
    spread = cumulative[:, None, :] - cumulative[None, :, :] + in_gate[None, :, :]
    spread = jnp.where(causal[:, :, None], spread, floor_neg)
    carried_log = cumulative + state_max[None, :]
    running = jnp.maximum(carried_log, lax.optimization_barrier(jnp.max(spread, axis=1)))
    carried = jnp.exp(carried_log - running)
    scores = jnp.einsum('thd,shd->tsh', queries, key_rows, precision=peak_value) * jnp.exp(spread - running[:, None, :])
    numerator = carried[:, :, None] * jnp.einsum('thd,hde->the', queries, state_matrix, precision=peak_value)
    numerator = numerator + jnp.einsum('tsh,she->the', scores, value_rows, precision=peak_value)
    block_total = cumulative[-1]
    gap_logs = block_total[None, :] - cumulative + in_gate
    next_max = jnp.maximum(block_total + state_max, lax.optimization_barrier(jnp.max(gap_logs, axis=0)))
    decay_factor = jnp.exp(block_total + state_max - next_max)
    weights = jnp.exp(gap_logs - next_max[None, :])
    next_matrix = decay_factor[:, None, None] * state_matrix + jnp.einsum('sh,shd,she->hde', weights, key_rows, value_rows, precision=peak_value)
    return ((next_matrix, next_max), numerator)

def memory_mixer(queries, key_rows, value_rows, log_forget, in_gate):
    segment_list = SEQ // BLOCK

    def split_blocks(array):
        return array.reshape((segment_list, BLOCK) + array.shape[1:])
    initial = (jnp.zeros((HM, DM, DM), jnp.float32), jnp.full((HM,), floor_neg, jnp.float32))
    scaled = key_rows * DM ** (-0.5)
    _, outputs = lax.scan(memory_block, initial, (split_blocks(queries), split_blocks(scaled), split_blocks(value_rows), split_blocks(log_forget), split_blocks(in_gate)))
    return outputs.reshape(SEQ, HM, DM)

def stick_piece(queries, key_rows, value_rows, head_bias, query_pos, key_start):
    logits = jnp.einsum('thd,shd->hts', queries.astype(jnp.float32), key_rows.astype(jnp.float32), precision=peak_value)
    logits = logits * DS ** (-0.5) + head_bias[:, None, None]
    key_pos = key_start + jnp.arange(key_rows.shape[0], dtype=jnp.int32)
    visible = key_pos[None, :] < query_pos[:, None]
    keep_log = jnp.where(visible[None], jax.nn.log_sigmoid(-logits), jnp.float32(0.0))
    after = lax.cumsum(keep_log, axis=2, reverse=True) - keep_log
    weights = jnp.where(visible[None], jnp.exp(jax.nn.log_sigmoid(logits) + after), jnp.float32(0.0)).astype(jnp.bfloat16)
    partial_out = jnp.einsum('hts,shd->thd', weights.astype(jnp.float32), value_rows.astype(jnp.float32), precision=peak_value)
    return (partial_out, lax.optimization_barrier(jnp.sum(keep_log, axis=2)).T)

def stick_mixer(queries, key_rows, value_rows, head_bias):

    def span_out(span):
        first_row = span * TOK_DEV
        query_span = lax.dynamic_slice_in_dim(queries, first_row, TOK_DEV, 0)
        query_pos = first_row + jnp.arange(TOK_DEV, dtype=jnp.int32)

        def visit(offset, state_carry):
            accumulated, running_sum = state_carry
            key_start = ((span - offset) * TOK_DEV).astype(jnp.int32)
            keys_span = lax.dynamic_slice_in_dim(key_rows, key_start, TOK_DEV, 0)
            values_span = lax.dynamic_slice_in_dim(value_rows, key_start, TOK_DEV, 0)
            part_out, part_keep = stick_piece(query_span, keys_span, values_span, head_bias, query_pos, key_start)
            return (accumulated + jnp.exp(running_sum)[:, :, None] * part_out, running_sum + part_keep)
        initial = (jnp.zeros((TOK_DEV, HS, DS), jnp.float32), jnp.zeros((TOK_DEV, HS), jnp.float32))
        accumulated, _ = lax.fori_loop(0, span + 1, visit, initial)
        return accumulated
    outputs = lax.map(span_out, jnp.arange(N_SP, dtype=jnp.int32))
    return outputs.reshape(SEQ, HS, DS)

def reference(tokens, norm_gain, memory_query, memory_key, memory_value, memory_outgate, memory_ingate, memory_forget, forget_bias, forget_shift, stick_query, stick_key, stick_value, stick_bias, memory_gain, stick_gain, out_memory, out_stick):

    def one_sequence(inputs):
        rows_in, shift_rows = inputs
        values = rows_in.astype(jnp.float32)
        normed = (values * lax.rsqrt(lax.optimization_barrier(jnp.mean(values * values, axis=-1, keepdims=True)) + epsilon) * norm_gain).astype(jnp.bfloat16)

        def project(weight):
            return jnp.dot(normed, weight, preferred_element_type=jnp.float32)
        memory_shape = (SEQ, HM, DM)
        queries = rounded(project(memory_query)).reshape(memory_shape)
        key_rows = rounded(project(memory_key)).reshape(memory_shape)
        value_rows = rounded(project(memory_value)).reshape(memory_shape)
        out_gate = jax.nn.sigmoid(rounded(project(memory_outgate))).reshape(memory_shape)
        in_gate = project(memory_ingate)
        log_forget = jax.nn.log_sigmoid(project(memory_forget) + forget_bias) + shift_rows
        memory_out = memory_mixer(queries, key_rows, value_rows, log_forget, in_gate)
        mix_memory = per_head_norm(out_gate * memory_out, memory_gain.reshape(HM, DM)).reshape(SEQ, HM * DM).astype(jnp.bfloat16)
        stick_shape = (SEQ, HS, DS)
        stick_q = project(stick_query).astype(jnp.bfloat16).reshape(stick_shape)
        stick_k = project(stick_key).astype(jnp.bfloat16).reshape(stick_shape)
        stick_v = project(stick_value).astype(jnp.bfloat16).reshape(stick_shape)
        stick_out = stick_mixer(stick_q, stick_k, stick_v, stick_bias)
        mix_stick = per_head_norm(stick_out, stick_gain.reshape(HS, DS)).reshape(SEQ, HS * DS).astype(jnp.bfloat16)
        mixed = jnp.dot(mix_memory, out_memory, preferred_element_type=jnp.float32) + jnp.dot(mix_stick, out_stick, preferred_element_type=jnp.float32)
        return mixed.astype(jnp.bfloat16)
    return lax.map(one_sequence, (tokens, forget_shift))
```

```python
import math

import jax
import jax.numpy as jnp
from jax import lax
from jax.experimental import pallas as pl
from jax.experimental.pallas import tpu as pltpu
from jax.sharding import Mesh
from jax.sharding import PartitionSpec as P


NZ, NY, NX, NT = 8, 4, 4, 2
SIZES = {"z": NZ, "y": NY, "fs": NX, "tp": NT}
D = 2048
TOK = 256
HD = 2
DM = 256
DS = 128
QR = DM // NY
ROWS = HD * QR + 16
FEAT = D // NX
epsilon = 1e-06
floor_neg = -1e30
LOG2E = 1.0 / math.log(2.0)
f32, bf16 = jnp.float32, jnp.bfloat16
NT_DIMS = (((1,), (1,)), ((), ()))
TN_DIMS = (((0,), (0,)), ((), ()))


def shift(array, axis, by):
    n = SIZES[axis]
    return lax.ppermute(array, axis, [(i, (i + by) % n) for i in range(n)])


def shift_up(array, axis, by):
    n = SIZES[axis]
    return lax.ppermute(array, axis, [(i, i + by) for i in range(n - by)])


def call(kernel, outs, *args, scratch=(), mib=48):
    return pl.pallas_call(
        kernel,
        out_shape=[jax.ShapeDtypeStruct(s, d) for s, d in outs],
        in_specs=[pl.BlockSpec(memory_space=pltpu.VMEM)] * len(args),
        out_specs=[pl.BlockSpec(memory_space=pltpu.VMEM)] * len(outs),
        scratch_shapes=list(scratch),
        compiler_params=pltpu.CompilerParams(vmem_limit_bytes=mib * 2**20),
        name=kernel.__name__,
    )(*args)


def log_sigmoid(x):
    return -(jnp.maximum(-x, 0.0) + jnp.log1p(jnp.exp(-jnp.abs(x))))


def iota(shape, dim):
    return lax.broadcasted_iota(jnp.int32, shape, dim)


def front(own, other, gain, wq, wk, wv, wg, wgt, fb, fbt, sh, sht,
          nrm4, q, kv, ccol, icol, crow, irow, full):
    t = lax.axis_index("tp")
    a = own[...].astype(f32)
    b = other[...].astype(f32)
    square = jnp.sum(a * a, axis=1, keepdims=True) + jnp.sum(b * b, axis=1, keepdims=True)
    scale = lax.rsqrt(square * (1.0 / D) + epsilon)
    low = jnp.where(t == 0, a, b)
    high = jnp.where(t == 0, b, a)
    full[:, : D // 2] = (low * scale * gain[:, : D // 2]).astype(bf16)
    full[:, D // 2 :] = (high * scale * gain[:, D // 2 :]).astype(bf16)
    for i in range(NX):
        nrm4[i] = full[:, i * FEAT : (i + 1) * FEAT]
    n = full[...]
    q[...] = jnp.dot(n, wq[...], preferred_element_type=f32).astype(bf16)
    kv[:, : HD * DS] = jnp.dot(n, wk[...], preferred_element_type=f32).astype(bf16)
    kv[:, HD * DS :] = jnp.dot(n, wv[...], preferred_element_type=f32).astype(bf16)
    gate = jnp.dot(n, wg[...], preferred_element_type=f32)
    gate_t = lax.dot_general(wgt[...], n, NT_DIMS, preferred_element_type=f32)
    lf = log_sigmoid(gate[:, HD : 2 * HD] + fb[...]) + sh[...]
    lf_t = log_sigmoid(gate_t[HD : 2 * HD, :] + fbt[...]) + sht[...]
    row, col = iota((TOK, TOK), 0), iota((TOK, TOK), 1)
    ccol[...] = jnp.dot((col <= row).astype(f32), lf, preferred_element_type=f32,
                        precision=lax.Precision.HIGHEST)
    crow[...] = jnp.dot(lf_t, (row <= col).astype(f32), preferred_element_type=f32,
                        precision=lax.Precision.HIGHEST)
    icol[...] = gate[:, :HD]
    irow[...] = gate_t[:HD, :]


def store_logs(ref, scalars):
    rows = iota((16, DM), 0)
    block = jnp.zeros((16, DM), f32)
    for i, s in enumerate(scalars):
        high = s.astype(bf16).astype(f32)
        middle = (s - high).astype(bf16).astype(f32)
        low = s - high - middle
        block = jnp.where(rows == 3 * i, high, block)
        block = jnp.where(rows == 3 * i + 1, middle, block)
        block = jnp.where(rows == 3 * i + 2, low, block)
    ref[HD * QR :, :] = block.astype(bf16)


def load_logs(ref, count):
    block = ref[HD * QR :, :].astype(f32)
    return [
        block[3 * i : 3 * i + 1, :] + block[3 * i + 1 : 3 * i + 2, :] + block[3 * i + 2 : 3 * i + 3, :]
        for i in range(count)
    ]


def project_rows(nrm4, pieces):
    x = lax.axis_index("fs")
    total = None
    for by, w in zip((0, 3, 1, 2), pieces):
        part = jnp.dot(nrm4[lax.rem(x + by, NX)], w[...], preferred_element_type=f32)
        total = part if total is None else total + part
    return total.astype(bf16)


def summary(nrm4, k0, k1, k2, k3, v0, v1, v2, v3, ccol, icol,
            mk, mv, m0, m1, m2, m3, state):
    y = lax.axis_index("y")
    mk[...] = project_rows(nrm4, (k0, k1, k2, k3)) * bf16(DM ** -0.5)
    mv[...] = project_rows(nrm4, (v0, v1, v2, v3))
    logs = []
    for h in range(HD):
        c = ccol[:, h : h + 1]
        total = ccol[TOK - 1 : TOK, h : h + 1]
        gap = total - c + icol[:, h : h + 1]
        top = jnp.max(gap, axis=0, keepdims=True)
        lanes = slice(h * DM, (h + 1) * DM)
        weighted = (mv[:, lanes].astype(f32) * jnp.exp(gap - top)).astype(bf16)
        state[h] = lax.dot_general(mk[:, lanes], weighted, TN_DIMS, preferred_element_type=f32)
        logs += [total, top]
    for by, ref in zip((0, 1, 2, 3), (m0, m1, m2, m3)):
        start = pl.multiple_of(lax.rem(y + by, NY) * QR, QR)
        for h in range(HD):
            ref[h * QR : (h + 1) * QR, :] = state[h, pl.ds(start, QR), :].astype(bf16)
        store_logs(ref, logs)


def y_logs(refs):
    logs = [load_logs(r, 2 * HD) for r in refs]
    totals = [[logs[d][2 * h] for d in range(NY)] for h in range(HD)]
    tops = [[logs[d][2 * h + 1] for d in range(NY)] for h in range(HD)]
    return totals, tops


def group(s0, s1, s2, s3, out):
    refs = (s0, s1, s2, s3)
    y = lax.axis_index("y")
    at = [lax.rem(y + NY - d, NY) for d in range(NY)]
    totals, tops = y_logs(refs)
    logs = []
    for h in range(HD):
        all_total = sum(totals[h])
        reach = []
        for d in range(NY):
            r = tops[h][d]
            for e in range(NY):
                r = r + jnp.where(at[e] > at[d], totals[h][e], 0.0)
            reach.append(r)
        top = jnp.maximum(jnp.maximum(reach[0], reach[1]), jnp.maximum(reach[2], reach[3]))
        rows = slice(h * QR, (h + 1) * QR)
        mixed = sum(jnp.exp(reach[d] - top) * refs[d][rows, :].astype(f32) for d in range(NY))
        out[rows, :] = mixed.astype(bf16)
        logs += [all_total[:, :1], top[:, :1]]
    store_logs(out, logs)


def incoming(s0, s1, s2, s3, g1, g2, g3, g4, g5, g6, g7, o0, o1, o2, o3):
    refs, groups = (s0, s1, s2, s3), (g1, g2, g3, g4, g5, g6, g7)
    y, z = lax.axis_index("y"), lax.axis_index("z")
    at = [lax.rem(y + NY - d, NY) for d in range(NY)]
    totals, tops = y_logs(refs)
    glogs = [load_logs(g, 2 * HD) for g in groups]
    outs = (o0, o1, o2, o3)
    logs = [[] for _ in outs]
    for h in range(HD):
        rows = slice(h * QR, (h + 1) * QR)
        reach, past = [], jnp.zeros((1, DM), f32)
        for d in range(1, NZ):
            there = z >= d
            reach.append(jnp.where(there, glogs[d - 1][2 * h + 1] + past, floor_neg))
            past = past + jnp.where(there, glogs[d - 1][2 * h], 0.0)
        gtop = reach[0]
        for r in reach[1:]:
            gtop = jnp.maximum(gtop, r)
        before = jnp.zeros((QR, DM), f32)
        for d in range(1, NZ):
            weight = jnp.where(z >= d, jnp.exp(reach[d - 1] - gtop), 0.0)
            before = before + weight * groups[d - 1][rows, :].astype(f32)
        for by, out in enumerate(outs):
            to = lax.rem(y + by, NY)
            own_reach = gtop
            for e in range(NY):
                own_reach = own_reach + jnp.where(at[e] < to, totals[h][e], 0.0)
            near = []
            for d in range(NY):
                r = tops[h][d]
                for e in range(NY):
                    r = r + jnp.where((at[e] > at[d]) & (at[e] < to), totals[h][e], 0.0)
                near.append(jnp.where(at[d] < to, r, floor_neg))
            top = own_reach
            for r in near:
                top = jnp.maximum(top, r)
            mixed = jnp.exp(own_reach - top) * before
            for d in range(NY):
                weight = jnp.where(at[d] < to, jnp.exp(near[d] - top), 0.0)
                mixed = mixed + weight * refs[d][rows, :].astype(f32)
            out[rows, :] = mixed.astype(bf16)
            logs[by].append(top[:, :1])
    for by, out in enumerate(outs):
        store_logs(out, logs[by])


def memory_out(nrm4, q0, q1, q2, q3, w0, w1, w2, w3, mk, mv, ccol, crow, irow, gain,
               s0, s1, s2, s3, keep, send, state, mixed):
    y, t = lax.axis_index("y"), lax.axis_index("tp")
    for d, ref in enumerate((s0, s1, s2, s3)):
        start = pl.multiple_of(lax.rem(y + NY - d, NY) * QR, QR)
        for h in range(HD):
            state[h, pl.ds(start, QR), :] = ref[h * QR : (h + 1) * QR, :]
    tops = load_logs(s0, HD)
    mq = project_rows(nrm4, (q0, q1, q2, q3))
    mo = project_rows(nrm4, (w0, w1, w2, w3))
    causal = iota((TOK, TOK), 1) <= iota((TOK, TOK), 0)
    for h in range(HD):
        lanes = slice(h * DM, (h + 1) * DM)
        qh = mq[:, lanes]
        c = ccol[:, h : h + 1]
        spread = c + (irow[h : h + 1, :] - crow[h : h + 1, :])
        spread = jnp.where(causal, spread, floor_neg)
        carried = c + tops[h][:, :1]
        running = jnp.maximum(carried, jnp.max(spread, axis=1, keepdims=True))
        scores = lax.dot_general(qh, mk[:, lanes], NT_DIMS, preferred_element_type=f32)
        scores = (scores * jnp.exp(spread - running)).astype(bf16)
        value = jnp.exp(carried - running) * jnp.dot(qh, state[h], preferred_element_type=f32)
        value = value + jnp.dot(scores, mv[:, lanes], preferred_element_type=f32)
        value = value * jax.nn.sigmoid(mo[:, lanes].astype(f32))
        scale = lax.rsqrt(jnp.mean(value * value, axis=1, keepdims=True) + epsilon)
        mixed[:, lanes] = value * scale * gain[:, lanes]
    half = TOK // NT
    keep[...] = mixed[pl.ds(pl.multiple_of(t * half, half), half), :].astype(bf16)
    send[...] = mixed[pl.ds(pl.multiple_of((1 - t) * half, half), half), :].astype(bf16)


def stick_tile(q, k, v, bias, upper, visible):
    z2 = lax.dot_general(q, k, NT_DIMS, preferred_element_type=f32)
    z2 = z2 * (DS ** -0.5 * LOG2E) + bias
    soft = jnp.maximum(jnp.log2(1.0 + jnp.exp2(jnp.minimum(z2, 120.0))), z2)
    rest = z2 - soft
    if visible is not None:
        soft = jnp.where(visible, soft, 0.0)
    after = jnp.dot(soft.astype(bf16), upper, preferred_element_type=f32)
    weights = jnp.exp2(rest - after)
    if visible is not None:
        weights = jnp.where(visible, weights, 0.0)
    part = jnp.dot(weights.astype(bf16), v, preferred_element_type=f32)
    return part, jnp.sum(soft, axis=1, keepdims=True)


def stick_parts(q0, q1, q2, q3, k0, k1, k2, k3, k4, k5, k6, k7, bias, parts, kept, qall, acc):
    y, z = lax.axis_index("y"), lax.axis_index("z")
    for by, ref in zip((0, 3, 1, 2), (q0, q1, q2, q3)):
        qall[lax.rem(y + by, NY)] = ref[...]
    acc[...] = jnp.zeros(acc.shape, f32)
    row, col = iota((TOK, TOK), 0), iota((TOK, TOK), 1)
    upper = (row > col).astype(bf16)
    strict = col < row

    def block(j, at, kv, visible):
        for h in range(HD):
            lanes = slice(h * DS, (h + 1) * DS)
            vlanes = slice(HD * DS + h * DS, HD * DS + (h + 1) * DS)
            part, soft = stick_tile(
                qall[j, :, lanes], kv[:, lanes], kv[:, vlanes],
                bias[:, h : h + 1] * LOG2E, upper, visible,
            )
            rows = pl.ds(pl.multiple_of(j * TOK, TOK), TOK)
            parts[at, rows, lanes] = part.astype(bf16)
            lane = iota((TOK, 128), 1)
            acc[j] = jnp.where(lane == at * HD + h, soft, acc[j])

    for by, kv in zip((0, 7, 6, 5, 4, 1, 2, 3), (k0, k1, k2, k3, k4, k5, k6, k7)):
        at = lax.rem(z + by, NZ)
        if by == 0:
            def own(j, _):
                @pl.when(j == y)
                def _():
                    block(j, at, kv, strict)

                @pl.when(j > y)
                def _():
                    block(j, at, kv, None)

                @pl.when(j < y)
                def _():
                    rows = pl.ds(pl.multiple_of(j * TOK, TOK), TOK)
                    parts[at, rows, :] = jnp.zeros((TOK, HD * DS), bf16)
                return 0

            lax.fori_loop(0, NY, own, 0)
        else:
            @pl.when(at < z)
            def _():
                def other(j, _):
                    block(j, at, kv, None)
                    return 0

                lax.fori_loop(0, NY, other, 0)
    for j in range(NY):
        kept[:, j * TOK : (j + 1) * TOK] = acc[j].T[: NZ * HD, :]


def stick_combine(parts, e0, e1, e2, e3, o0, o1, o2, o3, off, acc):
    y, z = lax.axis_index("y"), lax.axis_index("z")
    off[...] = jnp.zeros(off.shape, f32)
    run = jnp.zeros((HD, NY * TOK), f32)
    refs = (e0, e1, e2, e3)
    at = [lax.rem(y + by, NY) for by in (0, 3, 1, 2)]
    for i in range(NZ - 1, -1, -1):
        rows = slice(i * HD, (i + 1) * HD)
        later = run
        for d in range(NY):
            later = later + jnp.where(at[d] > y, refs[d][rows, :], 0.0)
            run = run + refs[d][rows, :]
        off[rows, :] = jnp.exp2(-later)
    acc[...] = jnp.zeros(acc.shape, f32)
    for j in range(NY):
        weight = off[:, j * TOK : (j + 1) * TOK].T
        rows = slice(j * TOK, (j + 1) * TOK)
        for i in range(NZ):
            @pl.when(i <= z)
            def _():
                for h in range(HD):
                    lanes = slice(h * DS, (h + 1) * DS)
                    acc[j, :, lanes] += weight[:, i * HD + h : i * HD + h + 1] * parts[
                        i, rows, lanes
                    ].astype(f32)
    for by, out in enumerate((o0, o1, o2, o3)):
        out[...] = acc[lax.rem(y + by, NY)].astype(bf16)


def stick_norm(a0, a1, a2, a3, gain, keep, send, mixed):
    t = lax.axis_index("tp")
    total = a0[...].astype(f32) + a1[...].astype(f32) + a2[...].astype(f32) + a3[...].astype(f32)
    for h in range(HD):
        lanes = slice(h * DS, (h + 1) * DS)
        value = total[:, lanes]
        scale = lax.rsqrt(jnp.mean(value * value, axis=1, keepdims=True) + epsilon)
        mixed[:, lanes] = value * scale * gain[:, lanes]
    half = TOK // NT
    keep[...] = mixed[pl.ds(pl.multiple_of(t * half, half), half), :].astype(bf16)
    send[...] = mixed[pl.ds(pl.multiple_of((1 - t) * half, half), half), :].astype(bf16)


def project_out(mm, ms, om, os_, wm, ws, owm, ows, out):
    total = jnp.dot(mm[...], wm[...], preferred_element_type=f32)
    total = total + jnp.dot(ms[...], ws[...], preferred_element_type=f32)
    total = total + jnp.dot(om[...], owm[...], preferred_element_type=f32)
    total = total + jnp.dot(os_[...], ows[...], preferred_element_type=f32)
    out[...] = total.astype(bf16)


def weight_ring(a, b):
    a_up, b_up = shift(a, "fs", 1), shift(b, "fs", 1)
    a_down, b_down = shift(a, "fs", -1), shift(b, "fs", -1)
    return (a, a_up, a_down, shift(a_up, "fs", 1)), (b, b_up, b_down, shift(b_down, "fs", -1))


def per_device(
    tokens, norm_gain, memory_query, memory_key, memory_value, memory_outgate, memory_ingate,
    memory_forget, forget_bias, forget_shift, stick_query, stick_key, stick_value, stick_bias,
    memory_gain, stick_gain, out_memory, out_stick,
):
    own = tokens[0]
    other = shift(own, "tp", 1)
    keys, values = weight_ring(memory_key, memory_value)
    queries, gates = weight_ring(memory_query, memory_outgate)
    far_memory, far_stick = shift(out_memory, "tp", 1), shift(out_stick, "tp", 1)

    wg = jnp.concatenate([memory_ingate, memory_forget], axis=1)
    wg = jnp.pad(wg, ((0, 0), (0, 4)))
    sh = forget_shift[0]
    nrm4, q, kv, ccol, icol, crow, irow = call(
        front,
        [((NX, TOK, FEAT), bf16), ((TOK, HD * DS), bf16), ((TOK, 2 * HD * DS), bf16),
         ((TOK, HD), f32), ((TOK, HD), f32), ((HD, TOK), f32), ((HD, TOK), f32)],
        own, other, norm_gain[None], stick_query, stick_key, stick_value, wg, wg.T,
        forget_bias[None], forget_bias[:, None], sh, sh.T,
        scratch=[pltpu.VMEM((TOK, D), bf16)],
    )

    qs = (q, shift(q, "y", 1), shift(q, "y", -1), shift(q, "y", 2))
    ups, downs = [kv], [kv]
    for _ in range(4):
        ups.append(shift(ups[-1], "z", 1))
        if len(downs) < 4:
            downs.append(shift(downs[-1], "z", -1))
    parts, kept = call(
        stick_parts,
        [((NZ, NY * TOK, HD * DS), bf16), ((NZ * HD, NY * TOK), f32)],
        *qs, *ups, *downs[1:], stick_bias[None],
        scratch=[pltpu.VMEM((NY, TOK, HD * DS), bf16), pltpu.VMEM((NY, TOK, 128), f32)],
    )
    keeps = (kept, shift(kept, "y", 1), shift(kept, "y", -1), shift(kept, "y", 2))
    o0, o1, o2, o3 = call(
        stick_combine, [((TOK, HD * DS), bf16)] * 4, parts, *keeps,
        scratch=[pltpu.VMEM((128, NY * TOK), f32), pltpu.VMEM((NY, TOK, HD * DS), f32)],
    )
    half = TOK // NT
    ms, ms_send = call(
        stick_norm, [((half, HD * DS), bf16)] * 2,
        o0, shift(o1, "y", 1), shift(o2, "y", 2), shift(o3, "y", -1), stick_gain[None],
        scratch=[pltpu.VMEM((TOK, HD * DS), f32)],
    )

    mk, mv, m0, m1, m2, m3 = call(
        summary,
        [((TOK, HD * DM), bf16)] * 2 + [((ROWS, DM), bf16)] * 4,
        nrm4, *keys, *values, ccol, icol,
        scratch=[pltpu.VMEM((HD, DM, DM), f32)],
    )
    slots = (m0, shift(m1, "y", 1), shift(m2, "y", 2), shift(m3, "y", -1))
    (g,) = call(group, [((ROWS, DM), bf16)], *slots)
    gs = tuple(shift_up(g, "z", d) for d in range(1, NZ))
    i0, i1, i2, i3 = call(incoming, [((ROWS, DM), bf16)] * 4, *slots, *gs)
    states = (i0, shift(i1, "y", 1), shift(i2, "y", 2), shift(i3, "y", -1))
    mm, mm_send = call(
        memory_out, [((half, HD * DM), bf16)] * 2,
        nrm4, *queries, *gates, mk, mv, ccol, crow, irow, memory_gain[None], *states,
        scratch=[pltpu.VMEM((HD, DM, DM), bf16), pltpu.VMEM((TOK, HD * DM), f32)],
    )

    (out,) = call(
        project_out, [((half, D), bf16)],
        mm, ms, shift(mm_send, "tp", 1), shift(ms_send, "tp", 1),
        out_memory, out_stick, far_memory, far_stick,
    )
    return out[None]


def solution(mesh):
    finer = Mesh(
        mesh.devices.reshape(NZ, NY, mesh.shape["fs"], mesh.shape["tp"]), ("z", "y", "fs", "tp")
    )
    sp = ("z", "y")
    return jax.shard_map(
        per_device,
        mesh=finer,
        in_specs=(
            P("fs", sp, "tp"), P(), P("fs", "tp"), P("fs", "tp"), P("fs", "tp"), P("fs", "tp"),
            P(None, "tp"), P(None, "tp"), P("tp"), P("fs", sp, "tp"), P(None, "tp"),
            P(None, "tp"), P(None, "tp"), P("tp"), P("tp"), P("tp"), P("tp", None), P("tp", None),
        ),
        out_specs=P("fs", ("z", "y", "tp"), None),
        check_vma=False,
    )
```
